32 devices in a mesh: sp: 8 (over z, x), tp: 4 (over y, core).
Axes of the slice: x: 2, y: 2, z: 4, core: 2. Of those that a mesh axis runs over, the one named last changes fastest.
Arguments:
- tokens: bfloat16 [6144, 2048], P(('sp', 'tp')), may hold values from -6 to 6
- norm_gain: bfloat16 [2048], replicated, may hold values from 0.099609375 to 1.8984375
- conv_value_w: bfloat16 [2048, 2048], P('sp', 'tp'), may hold values from -0.125 to 0.125
- conv_gate_w: bfloat16 [2048, 2048], P('sp', 'tp'), may hold values from -0.125 to 0.125
- rnn_input_w: bfloat16 [2048, 2560], P('sp', 'tp'), may hold values from -0.125 to 0.125
- rnn_gate_w: bfloat16 [2048, 2560], P('sp', 'tp'), may hold values from -0.125 to 0.125
- conv_kernel: bfloat16 [31, 2048], P(None, 'tp'), may hold values from -3 to 3
- conv_norm_gain: bfloat16 [2048], P('tp'), may hold values from 0.099609375 to 1.8984375
- conv_norm_shift: bfloat16 [2048], P('tp'), may hold values from -3 to 3
- short_kernel: bfloat16 [4, 2560], P(None, 'tp'), may hold values from -3 to 3
- recur_map: bfloat16 [16, 160, 160], P('tp'), may hold values from -0.5 to 0.5
- input_map: bfloat16 [16, 160, 160], P('tp'), may hold values from -0.5 to 0.5
- decay_param: float32 [2560], P('tp'), may hold values from 4.5 to 16
- decay_shift: float32 [6144, 16], P('sp', 'tp'), may hold values from -1.1 to 0
- initial_state: float32 [2560], P('tp'), may hold values from -5 to 5
- conv_out_w: bfloat16 [2048, 2048], P('tp', 'sp'), may hold values from -0.125 to 0.125
- rnn_out_w: bfloat16 [2560, 2048], P('tp', 'sp'), may hold values from -0.125 to 0.125
Outputs:
- mixed: bfloat16 [6144, 2048], P(('sp', 'tp'))
The draws below stay inside these ranges and needn't reach their ends.
All inputs are finite; a program needn't handle non-finite values.
Results may differ from the reference program's by a relative error of at most 0.015.
Values may be sent and summed in bfloat16 or wider, within the bound.
A program may use at most 128 MiB of HBM per device.

```python
import jax
import jax.numpy as jnp
from jax import lax

D = 2048
D_CONV = 2048
RNN_HEADS = 16
HEAD_DIM = 160
CONV_WIDTH = 31
SHORT_WIDTH = 4
TOK_DEV = 768
D_RNN = 2560
SEQUENCE_SPAN = 6144
N_TP = 4


def draw_conv_kernel(key, part):
    base = jnp.clip(jax.random.normal(jax.random.fold_in(key, 11), (CONV_WIDTH, D_CONV), jnp.float32), -4.0, 4.0)
    position = jnp.arange(D_CONV, dtype=jnp.float32) / D_CONV
    rough = jax.random.uniform(jax.random.fold_in(key, 12), (D_CONV,), jnp.float32, 0.5, 1.5)
    rising = jnp.exp(jnp.log(4.0) * position) / 2.0
    return (base * (rising * rough)[None, :] * CONV_WIDTH ** (-0.5)).astype(jnp.bfloat16)


def draw_decay_param(key, part):
    fast_heads = jax.random.randint(jax.random.fold_in(key, 21), (RNN_HEADS,), 0, 2) < 1
    fast_cols = jnp.repeat(fast_heads, HEAD_DIM)
    spread_draw = jax.random.uniform(jax.random.fold_in(key, 22), (D_RNN,), jnp.float32, 0.0, 1.0)
    slow_rate = jnp.exp(jnp.log(0.2) + spread_draw * jnp.log(4.0)) / SEQUENCE_SPAN
    fast_rate = jnp.exp(jnp.log(0.03) + spread_draw * jnp.log(0.08 / 0.03))
    rate = jnp.where(fast_cols, fast_rate, slow_rate)
    return -jnp.log(jnp.expm1(rate / 8.0))


def draw_decay_shift(key, part):
    sequence_indices = jnp.arange(SEQUENCE_SPAN, dtype=jnp.int32)
    span_len = max(TOK_DEV // 2, 1)
    span_count = (SEQUENCE_SPAN + span_len - 1) // span_len
    level_draw = jax.random.uniform(jax.random.fold_in(key, 31), (span_count,), jnp.float32, 0.0, 1.0)
    level = jnp.exp(jnp.log(0.1) + level_draw * jnp.log(10.0)) / SEQUENCE_SPAN
    baseline_amplitude = level[sequence_indices // span_len]
    spike_index = jax.random.randint(jax.random.fold_in(key, 32), (2,), 0, SEQUENCE_SPAN)
    objective_scalar = jax.random.uniform(jax.random.fold_in(key, 33), (2, RNN_HEADS), jnp.float32, 0.2, 0.4)
    match_tally = (sequence_indices[:, None] == spike_index[None, :]).astype(jnp.float32)
    spike_pattern = jnp.dot(match_tally, jnp.log1p(-objective_scalar))
    return spike_pattern - baseline_amplitude[:, None]


def steps_of(own_key, dims, pieces, low, top_value):
    gain = 1.0
    for dim, blocks in pieces:
        heights = jax.random.uniform(jax.random.fold_in(jax.random.fold_in(own_key, 6), dim), (blocks,), jnp.float32, low / len(pieces), top_value / len(pieces))
        gain = gain * jnp.repeat(jnp.exp(heights), dims[dim] // blocks).reshape((-1,) + (1,) * (len(dims) - 1 - dim))
    return gain


def scatter_about(own_key, shape, width, reach, split=(), kind=jnp.bfloat16):
    loudness = steps_of(own_key, shape, split, -0.22, 0.18) if split else 1.0
    drawn = jax.random.normal(own_key, shape, jnp.float32) * width * loudness
    return jnp.minimum(jnp.maximum(drawn, -reach), reach).astype(kind)


def setup_inputs(seed: int = 0) -> dict:
    key_list = jax.random.split(jax.random.key(seed), 18)
    tokens = scatter_about(key_list[0], (SEQUENCE_SPAN, D), 1.0, 6.0, ((0, 32),))
    norm_gain = jnp.clip(1.0 + 0.18 * jax.random.normal(key_list[1], (D,), jnp.float32), 0.099609375, 1.8984375).astype(jnp.bfloat16)
    conv_value_w = scatter_about(key_list[2], (D, D_CONV), D ** -0.5, 0.125, ((0, 8), (1, 4)))
    conv_gate_w = scatter_about(key_list[3], (D, D_CONV), D ** -0.5, 0.125, ((0, 8), (1, 4)))
    rnn_input_w = scatter_about(key_list[4], (D, D_RNN), D ** -0.5, 0.125, ((0, 8), (1, 4)))
    rnn_gate_w = scatter_about(key_list[5], (D, D_RNN), D ** -0.5, 0.125, ((0, 8), (1, 4)))
    conv_kernel = draw_conv_kernel(jax.random.fold_in(key_list[17], 71), 0)
    conv_norm_gain = jnp.clip(1.0 + 0.18 * jax.random.normal(key_list[7], (D_CONV,), jnp.float32), 0.099609375, 1.8984375).astype(jnp.bfloat16)
    conv_norm_shift = scatter_about(key_list[8], (D_CONV,), 0.5, 3.0, ((0, 4),))
    short_kernel = scatter_about(key_list[9], (SHORT_WIDTH, D_RNN), SHORT_WIDTH ** -0.5, 3.0, ((1, 4),))
    recur_map = scatter_about(key_list[10], (RNN_HEADS, HEAD_DIM, HEAD_DIM), HEAD_DIM ** -0.5, 0.5, ((0, 4),))
    input_map = scatter_about(key_list[11], (RNN_HEADS, HEAD_DIM, HEAD_DIM), HEAD_DIM ** -0.5, 0.5, ((0, 4),))
    decay_param = draw_decay_param(jax.random.fold_in(key_list[17], 71), 0)
    decay_shift = draw_decay_shift(jax.random.fold_in(key_list[17], 71), 0)
    initial_state = scatter_about(key_list[14], (D_RNN,), 1.0, 5.0, ((0, 4),), jnp.float32)
    conv_out_w = scatter_about(key_list[15], (D_CONV, D), D_CONV ** -0.5, 0.125, ((0, 4), (1, 8)))
    rnn_out_w = scatter_about(key_list[16], (D_RNN, D), D_RNN ** -0.5, 0.125, ((0, 4), (1, 8)))
    return dict(tokens=tokens, norm_gain=norm_gain, conv_value_w=conv_value_w, conv_gate_w=conv_gate_w, rnn_input_w=rnn_input_w, rnn_gate_w=rnn_gate_w, conv_kernel=conv_kernel, conv_norm_gain=conv_norm_gain, conv_norm_shift=conv_norm_shift, short_kernel=short_kernel, recur_map=recur_map, input_map=input_map, decay_param=decay_param, decay_shift=decay_shift, initial_state=initial_state, conv_out_w=conv_out_w, rnn_out_w=rnn_out_w)


EPS = 1e-06
EXPONENT = 8.0

def causal_taps(extended, kernel, length):
    result = jnp.zeros((length, extended.shape[1]), jnp.float32)
    for offset in range(kernel.shape[0]):
        result = result + kernel[offset].astype(jnp.float32) * extended[offset:offset + length]
    return result

def linear_pair(earlier, later):
    return (earlier[0] * later[0], later[0] * earlier[1] + later[1])

def block_diagonal(values, maps):
    row_count = values.shape[0]
    grouped = values.reshape(row_count, maps.shape[0], maps.shape[1]).astype(jnp.float32)
    mapped = jnp.einsum('rhi,hij->rhj', grouped, maps.astype(jnp.float32))
    return mapped.reshape(row_count, -1)

def reference(tokens, norm_gain, conv_value_w, conv_gate_w, rnn_input_w, rnn_gate_w, conv_kernel, conv_norm_gain, conv_norm_shift, short_kernel, recur_map, input_map, decay_param, decay_shift, initial_state, conv_out_w, rnn_out_w):
    length = TOK_DEV
    block_count = SEQUENCE_SPAN // length
    conv_reach = CONV_WIDTH - 1
    short_reach = SHORT_WIDTH - 1
    soft_rate = jax.nn.softplus(-decay_param)
    conv_group = D_CONV // N_TP
    rnn_group = D_RNN // N_TP

    def advance(carried, inputs):
        value_tail, gate_tail, input_tail, state = carried
        block_rows, block_shift = inputs
        as_float = block_rows.astype(jnp.float32)
        scale = lax.rsqrt(lax.optimization_barrier(jnp.mean(as_float * as_float, axis=1, keepdims=True)) + EPS)
        normed = (as_float * scale * norm_gain.astype(jnp.float32)).astype(jnp.bfloat16)
        conv_value = jnp.dot(normed, conv_value_w, preferred_element_type=jnp.float32).astype(jnp.bfloat16)
        conv_gate = jnp.dot(normed, conv_gate_w, preferred_element_type=jnp.float32).astype(jnp.bfloat16)
        rnn_input = jnp.dot(normed, rnn_input_w, preferred_element_type=jnp.float32).astype(jnp.bfloat16)
        rnn_gate = jnp.dot(normed, rnn_gate_w, preferred_element_type=jnp.float32).astype(jnp.bfloat16)
        value_ext = jnp.concatenate([value_tail, conv_value], axis=0)
        gate_ext = jnp.concatenate([gate_tail, conv_gate], axis=0)
        input_ext = jnp.concatenate([input_tail, rnn_input], axis=0)
        gated_values = value_ext.astype(jnp.float32) * jax.nn.sigmoid(gate_ext.astype(jnp.float32))
        conv_mixed = causal_taps(gated_values, conv_kernel, length)
        average = lax.optimization_barrier(jnp.mean(conv_mixed, axis=1, keepdims=True))
        spread = lax.optimization_barrier(jnp.mean(conv_mixed * conv_mixed, axis=1, keepdims=True)) - average * average
        scaled = (conv_mixed - average) * lax.rsqrt(spread + EPS)
        scaled = scaled * conv_norm_gain.astype(jnp.float32) + conv_norm_shift.astype(jnp.float32)
        conv_hidden = jax.nn.silu(scaled).astype(jnp.bfloat16)
        rnn_short = causal_taps(input_ext.astype(jnp.float32), short_kernel, length).astype(jnp.bfloat16)
        recur_gate = jax.nn.sigmoid(block_diagonal(rnn_short, recur_map))
        input_gate = jax.nn.sigmoid(block_diagonal(rnn_short, input_map))
        shift_cols = jnp.repeat(block_shift, HEAD_DIM, axis=1)
        log_decay = -EXPONENT * recur_gate * soft_rate[None, :] + shift_cols
        drive = jnp.sqrt(-jnp.expm1(2.0 * log_decay)) * input_gate * rnn_short.astype(jnp.float32)
        cum_decay, cum_drive = lax.associative_scan(linear_pair, (jnp.exp(log_decay), drive), axis=0)
        states = cum_drive + cum_decay * state[None, :]
        rnn_hidden = (states * jax.nn.gelu(rnn_gate.astype(jnp.float32), approximate=True)).astype(jnp.bfloat16)
        result = jnp.zeros((length, D), jnp.float32)
        for group in range(N_TP):
            conv_lo = group * conv_group
            rnn_lo = group * rnn_group
            partial_value = jnp.dot(conv_hidden[:, conv_lo:conv_lo + conv_group], conv_out_w[conv_lo:conv_lo + conv_group], preferred_element_type=jnp.float32)
            partial_value = partial_value + jnp.dot(rnn_hidden[:, rnn_lo:rnn_lo + rnn_group], rnn_out_w[rnn_lo:rnn_lo + rnn_group], preferred_element_type=jnp.float32)
            rounded = lax.optimization_barrier(partial_value.astype(jnp.bfloat16))
            result = result + rounded.astype(jnp.float32)
        carried_next = (value_ext[value_ext.shape[0] - conv_reach:], gate_ext[gate_ext.shape[0] - conv_reach:], input_ext[input_ext.shape[0] - short_reach:], states[length - 1])
        return (carried_next, result.astype(jnp.bfloat16))
    start_carry = (jnp.zeros((conv_reach, D_CONV), jnp.bfloat16), jnp.zeros((conv_reach, D_CONV), jnp.bfloat16), jnp.zeros((short_reach, D_RNN), jnp.bfloat16), initial_state.astype(jnp.float32))
    blocks_in = (tokens.reshape(block_count, length, D), decay_shift.reshape(block_count, length, RNN_HEADS))
    final_carry, outputs = lax.scan(advance, start_carry, blocks_in)
    return outputs.reshape(SEQUENCE_SPAN, D)
```

```python
import functools

import jax
import jax.numpy as jnp
from jax import lax
from jax.experimental import pallas as pl
from jax.experimental.pallas import tpu as pltpu
from jax.sharding import PartitionSpec as P

EPS = 1e-06
EXPONENT = 8.0


def shifted(x, axis, by):
    peers = lax.axis_size(axis)
    pairs = [(i, i + by) for i in range(peers) if 0 <= i + by < peers]
    return lax.ppermute(x, axis, pairs)


def send_to(src, dst, send, recv, axis, peer):
    return pltpu.make_async_remote_copy(
        src_ref=src,
        dst_ref=dst,
        send_sem=send,
        recv_sem=recv,
        device_id={axis: peer},
        device_id_type=pl.DeviceIdType.MESH,
    )


def project_kernel(n, m, x_ref, w_ref, o_ref, blocks, piece, acc, ring_send, ring_recv, tok_send, tok_recv, own_sem):
    half = n // 2
    me = lax.axis_index("sp")
    lane = lax.axis_index("tp")
    at = jnp.where(me % 2 == 0, me // 2, n - 1 - me // 2)

    def device_at(place):
        place = lax.rem(place + 2 * n, n)
        return jnp.where(place < half, 2 * place, 2 * (n - 1 - place) + 1)

    right = device_at(at + 1)
    left = device_at(at - 1)
    barrier = pltpu.get_barrier_semaphore()
    for peer in (left, right):
        pl.semaphore_signal(barrier, inc=1, device_id={"sp": peer}, device_id_type=pl.DeviceIdType.MESH)
    for i in range(1, m):
        pl.semaphore_signal(
            barrier, inc=1, device_id={"tp": lax.rem(lane + i, m)}, device_id_type=pl.DeviceIdType.MESH
        )
    own_w = pltpu.make_async_copy(w_ref, blocks.at[me], own_sem.at[0])
    own_x = pltpu.make_async_copy(x_ref, piece.at[lane], own_sem.at[1])
    own_w.start()
    own_x.start()
    own_w.wait()
    own_x.wait()
    pl.semaphore_wait(barrier, 2 + m - 1)
    rows = w_ref.shape[0] // 2

    def hop(way, k, part=None):
        slot = device_at(at - (k - 1)) if way == 0 else device_at(at + (k - 1))
        ref = blocks.at[slot] if part is None else blocks.at[slot, pl.ds(part * rows, rows)]
        return send_to(
            ref, ref, ring_send.at[way, k - 1], ring_recv.at[way, k - 1], "sp", right if way == 0 else left
        )

    tokens_out = [
        send_to(x_ref, piece.at[lane], tok_send.at[i - 1], tok_recv.at[i - 1], "tp", lax.rem(lane + i, m))
        for i in range(1, m)
    ]

    def add(slot, first=False):
        def one(j, _):
            here = pl.ds(pl.multiple_of(j * piece.shape[2], piece.shape[2]), piece.shape[2])
            term = jnp.dot(piece[j, slot], blocks[slot], preferred_element_type=jnp.float32)
            acc[here, :] = term if first else acc[here, :] + term
            return 0

        lax.fori_loop(0, m, one, 0)

    hop(0, 1).start()
    hop(1, 1).start()
    for copy in tokens_out:
        copy.start()
    hop(0, 1).wait_recv()
    hop(1, 1).wait_recv()
    hop(0, 2).start()
    hop(1, 2).start()
    for copy in tokens_out:
        copy.wait_recv()
    add(me, True)

    def step(k, _):
        add(device_at(at - (k - 1)))
        add(device_at(at + (k - 1)))
        hop(0, k).wait_recv()
        hop(1, k).wait_recv()

        @pl.when(k + 1 < half)
        def _():
            hop(0, k + 1).start()
            hop(1, k + 1).start()

        return 0

    lax.fori_loop(2, half, step, 0)
    hop(0, half, 0).start()
    hop(1, half, 1).start()
    add(device_at(at - (half - 1)))
    add(device_at(at + (half - 1)))
    hop(0, half, 0).wait_recv()
    hop(1, half, 1).wait_recv()
    add(device_at(at + half))

    def finish(j, _):
        here = pl.ds(pl.multiple_of(j * piece.shape[2], piece.shape[2]), piece.shape[2])
        o_ref[here, :] = acc[here, :].astype(o_ref.dtype)
        return 0

    lax.fori_loop(0, m, finish, 0)

    def sent(k, _):
        hop(0, k).wait_send()
        hop(1, k).wait_send()
        return 0

    lax.fori_loop(1, half, sent, 0)
    hop(0, half, 0).wait_send()
    hop(1, half, 1).wait_send()
    for copy in tokens_out:
        copy.wait_send()


def project(normed, weight):
    n = lax.axis_size("sp")
    m = lax.axis_size("tp")
    rows = normed.shape[0]
    depth, columns = weight.shape
    sliced = normed.reshape(rows, n, depth).transpose(1, 0, 2)
    vmem = pl.BlockSpec(memory_space=pltpu.VMEM)
    return pl.pallas_call(
        functools.partial(project_kernel, n, m),
        out_shape=jax.ShapeDtypeStruct((rows * m, columns), jnp.bfloat16),
        in_specs=[vmem, vmem],
        out_specs=vmem,
        scratch_shapes=[
            pltpu.VMEM((n, depth, columns), jnp.bfloat16),
            pltpu.VMEM((m, n, rows, depth), jnp.bfloat16),
            pltpu.VMEM((rows * m, columns), jnp.float32),
            pltpu.SemaphoreType.DMA((2, n // 2)),
            pltpu.SemaphoreType.DMA((2, n // 2)),
            pltpu.SemaphoreType.DMA((m - 1,)),
            pltpu.SemaphoreType.DMA((m - 1,)),
            pltpu.SemaphoreType.DMA((2,)),
        ],
        cost_estimate=pl.CostEstimate(
            flops=2 * rows * m * depth * n * columns, bytes_accessed=90_000_000, transcendentals=0
        ),
        compiler_params=pltpu.CompilerParams(
            collective_id=0, has_side_effects=True, vmem_limit_bytes=50 * 1024 * 1024
        ),
    )(sliced, weight)


def spread_kernel(n, axis, x_ref, o_ref, send, recv):
    me = lax.axis_index(axis)
    barrier = pltpu.get_barrier_semaphore()

    def greet(i, _):
        pl.semaphore_signal(
            barrier, inc=1, device_id={axis: lax.rem(me + i, n)}, device_id_type=pl.DeviceIdType.MESH
        )
        return 0

    lax.fori_loop(1, n, greet, 0)
    pl.semaphore_wait(barrier, n - 1)

    def copy(i):
        return send_to(x_ref, o_ref.at[me], send.at[i - 1], recv.at[i - 1], axis, lax.rem(me + i, n))

    def start(i, _):
        copy(i).start()
        return 0

    def wait(i, _):
        copy(i).wait()
        return 0

    lax.fori_loop(1, n, start, 0)
    o_ref[pl.ds(me, 1)] = x_ref[...][None]
    lax.fori_loop(1, n, wait, 0)


def spread_over(x, axis, collective_id):
    n = lax.axis_size(axis)
    vmem = pl.BlockSpec(memory_space=pltpu.VMEM)
    return pl.pallas_call(
        functools.partial(spread_kernel, n, axis),
        out_shape=jax.ShapeDtypeStruct((n,) + x.shape, x.dtype),
        in_specs=[vmem],
        out_specs=vmem,
        scratch_shapes=[pltpu.SemaphoreType.DMA((n - 1,)), pltpu.SemaphoreType.DMA((n - 1,))],
        cost_estimate=pl.CostEstimate(flops=0, bytes_accessed=10_000_000, transcendentals=0),
        compiler_params=pltpu.CompilerParams(
            collective_id=collective_id, has_side_effects=True, vmem_limit_bytes=4 * 1024 * 1024
        ),
    )(x)


def scan_kernel(parts, a_ref, b_ref, p_ref, h_ref):
    length, width = a_ref.shape
    run = length // parts
    cols = [slice(None)]

    def one(i, state):
        place = pl.ds(i, parts, stride=run)
        new = []
        for c, (p, h) in zip(cols, state):
            a = a_ref[place, c]
            h = a * h + b_ref[place, c]
            p = a * p
            p_ref[place, c] = p
            h_ref[place, c] = h
            new.append((p, h))
        return new

    first = [(jnp.ones((parts, width), jnp.float32), jnp.zeros((parts, width), jnp.float32)) for _ in cols]
    ends = lax.fori_loop(0, run, one, first)
    for c, (p, h) in zip(cols, ends):
        carry_p = p[0:1]
        carry_h = h[0:1]
        for s in range(1, parts):
            here = pl.ds(s * run, run)
            local_p = p_ref[here, c]
            h_ref[here, c] = h_ref[here, c] + local_p * carry_h
            p_ref[here, c] = local_p * carry_p
            carry_h = p[s : s + 1] * carry_h + h[s : s + 1]
            carry_p = p[s : s + 1] * carry_p


def scan(a, b):
    block = pl.BlockSpec((a.shape[0], 128), lambda c: (0, c))
    return pl.pallas_call(
        functools.partial(scan_kernel, 8),
        grid=(a.shape[1] // 128,),
        out_shape=[jax.ShapeDtypeStruct(a.shape, jnp.float32)] * 2,
        in_specs=[block, block],
        out_specs=[block, block],
        cost_estimate=pl.CostEstimate(flops=4 * a.size, bytes_accessed=16 * a.size, transcendentals=0),
        compiler_params=pltpu.CompilerParams(vmem_limit_bytes=20 * 1024 * 1024),
    )(a, b)


def entering(last_decay, last_drive, initial):
    n = lax.axis_size("sp")
    place = lax.axis_index("sp")
    pair = jnp.stack([last_decay, last_drive])
    gathered = spread_over(jnp.pad(pair, ((0, 6), (0, 0))), "sp", 1)
    state = initial
    for i in range(n):
        state = jnp.where(i < place, gathered[i, 0] * state + gathered[i, 1], state)
    return state


def causal_taps(extended, kernel, length):
    result = jnp.zeros((length, extended.shape[1]), jnp.float32)
    for offset in range(kernel.shape[0]):
        result = result + kernel[offset].astype(jnp.float32) * extended[offset : offset + length]
    return result


def block_diagonal(values, maps):
    heads, size, _ = maps.shape
    rows = [
        jnp.pad(maps[h], ((0, 0), (h * size, (heads - 1 - h) * size))) for h in range(heads)
    ]
    return jnp.dot(values, jnp.concatenate(rows, axis=0), preferred_element_type=jnp.float32)


def local(
    tokens,
    norm_gain,
    conv_value_w,
    conv_gate_w,
    rnn_input_w,
    rnn_gate_w,
    conv_kernel,
    conv_norm_gain,
    conv_norm_shift,
    short_kernel,
    recur_map,
    input_map,
    decay_param,
    decay_shift,
    initial_state,
    conv_out_w,
    rnn_out_w,
):
    as_float = tokens.astype(jnp.float32)
    scale = lax.rsqrt(jnp.mean(as_float * as_float, axis=1, keepdims=True) + EPS)
    normed = (as_float * scale * norm_gain.astype(jnp.float32)).astype(jnp.bfloat16)
    edges = [0]
    for weight in (conv_value_w, conv_gate_w, rnn_input_w, rnn_gate_w):
        edges.append(edges[-1] + weight.shape[1])
    joined = project(
        normed, jnp.concatenate([conv_value_w, conv_gate_w, rnn_input_w, rnn_gate_w], axis=1)
    )
    conv_value, conv_gate, rnn_input, rnn_gate = [
        joined[:, edges[index] : edges[index + 1]] for index in range(4)
    ]
    out_weights = (
        lax.all_gather(conv_out_w, "sp", axis=1, tiled=True),
        lax.all_gather(rnn_out_w, "sp", axis=1, tiled=True),
    )
    length = conv_value.shape[0]
    conv_reach = conv_kernel.shape[0] - 1
    short_reach = short_kernel.shape[0] - 1
    tail = shifted(joined[length - conv_reach :, : edges[3]], "sp", 1)
    value_tail = tail[:, : edges[1]]
    gate_tail = tail[:, edges[1] : edges[2]]
    input_tail = tail[conv_reach - short_reach :, edges[2] :]
    value_ext = jnp.concatenate([value_tail, conv_value], axis=0)
    gate_ext = jnp.concatenate([gate_tail, conv_gate], axis=0)
    input_ext = jnp.concatenate([input_tail, rnn_input], axis=0)
    gated_values = value_ext.astype(jnp.float32) * jax.nn.sigmoid(gate_ext.astype(jnp.float32))
    conv_mixed = causal_taps(gated_values, conv_kernel, length)
    moments = lax.psum(
        (jnp.sum(conv_mixed, axis=1), jnp.sum(conv_mixed * conv_mixed, axis=1)), "tp"
    )
    channels = conv_mixed.shape[1] * lax.axis_size("tp")
    average = moments[0][:, None] / channels
    spread = moments[1][:, None] / channels - average * average
    scaled = (conv_mixed - average) * lax.rsqrt(spread + EPS)
    scaled = scaled * conv_norm_gain.astype(jnp.float32) + conv_norm_shift.astype(jnp.float32)
    conv_hidden = jax.nn.silu(scaled).astype(jnp.bfloat16)
    rnn_short = causal_taps(input_ext.astype(jnp.float32), short_kernel, length).astype(
        jnp.bfloat16
    )
    recur_gate = jax.nn.sigmoid(block_diagonal(rnn_short, recur_map))
    input_gate = jax.nn.sigmoid(block_diagonal(rnn_short, input_map))
    shift_cols = jnp.repeat(decay_shift, recur_map.shape[1], axis=1)
    log_decay = -EXPONENT * recur_gate * jax.nn.softplus(-decay_param)[None, :] + shift_cols
    drive = jnp.sqrt(-jnp.expm1(2.0 * log_decay)) * input_gate * rnn_short.astype(jnp.float32)
    cum_decay, cum_drive = scan(jnp.exp(log_decay), drive)
    state_before = entering(cum_decay[length - 1], cum_drive[length - 1], initial_state)
    states = cum_drive + cum_decay * state_before[None, :]
    rnn_hidden = (states * jax.nn.gelu(rnn_gate.astype(jnp.float32), approximate=True)).astype(
        jnp.bfloat16
    )
    return lax.psum_scatter(
        (
            jnp.dot(conv_hidden, out_weights[0], preferred_element_type=jnp.float32)
            + jnp.dot(rnn_hidden, out_weights[1], preferred_element_type=jnp.float32)
        ).astype(jnp.bfloat16),
        "tp",
        scatter_dimension=0,
        tiled=True,
    )


def solution(mesh):
    return jax.shard_map(
        local,
        mesh=mesh,
        in_specs=(
            P(("sp", "tp"), None),
            P(),
            P("sp", "tp"),
            P("sp", "tp"),
            P("sp", "tp"),
            P("sp", "tp"),
            P(None, "tp"),
            P("tp"),
            P("tp"),
            P(None, "tp"),
            P("tp", None, None),
            P("tp", None, None),
            P("tp"),
            P("sp", "tp"),
            P("tp"),
            P("tp", "sp"),
            P("tp", "sp"),
        ),
        out_specs=P(("sp", "tp"), None),
        check_vma=False,
    )
```
